128 devices in a mesh: rep: 2 (over x_hi), fs: 16 (over y, x_lo, core), tp: 4 (over z).
Axes of the slice: x: 4 (x_hi: 2, x_lo: 2; x = x_hi * 2 + x_lo), y: 4, z: 4, core: 2. Of those that a mesh axis runs over, the one named last changes fastest.
Arguments:
- tokens: bfloat16 [16384, 2048], P(('rep', 'fs', 'tp')), may hold values from -3 to 3
- mixer_output: bfloat16 [16384, 2048], P(('rep', 'fs', 'tp')), may hold values from -6 to 6
- early_norm: float32 [2048], replicated, may hold values from 0.75 to 1.25
- early_gate: bfloat16 [2048, 5120], P('fs', 'tp'), may hold values from -0.125 to 0.125
- early_value: bfloat16 [2048, 5120], P('fs', 'tp'), may hold values from -0.125 to 0.125
- early_down: bfloat16 [5120, 2048], P('tp', 'fs'), may hold values from -0.078125 to 0.078125
- early_post: float32 [2048], replicated, may hold values from 0.75 to 1.25
- mixer_gain: float32 [2048], replicated, may hold values from 0.75 to 1.25
- later_norm: float32 [2048], replicated, may hold values from 0.75 to 1.25
- later_gate: bfloat16 [2048, 5120], P('fs', 'tp'), may hold values from -0.125 to 0.125
- later_value: bfloat16 [2048, 5120], P('fs', 'tp'), may hold values from -0.125 to 0.125
- later_down: bfloat16 [5120, 2048], P('tp', 'fs'), may hold values from -0.078125 to 0.078125
- later_post: float32 [2048], replicated, may hold values from 0.75 to 1.25
Outputs:
- layer_out: bfloat16 [16384, 2048], P(('rep', 'fs', 'tp'))
The draws below stay inside these ranges and needn't reach their ends.
All inputs are finite; a program needn't handle non-finite values.
Results may differ from the reference program's by a relative error of at most 0.015.
Values may be sent and summed in bfloat16 or wider, within the bound.
No kernel may reach another device: no remote copies, remote signals or barrier semaphores. Data moves between devices by JAX's collectives and lax.ppermute only.
A program may use at most 128 MiB of HBM per device.

```python
import jax
import jax.numpy as jnp
from jax import lax

D = 2048
FF = 5120
TOKENS = 16384


def steps_of(rng, extent, split, low, top_value):
    def one(position, parts):
        draws = jax.random.uniform(jax.random.fold_in(jax.random.fold_in(rng, 6), position), (parts,), jnp.float32, low / len(split), top_value / len(split))
        return jnp.repeat(jnp.exp(draws), extent[position] // parts).reshape((-1,) + (1,) * (len(extent) - position - 1))

    loudness = one(*split[0])
    for cut in split[1:]:
        loudness = loudness * one(*cut)
    return loudness


def scatter_about(stream_key, dims, scale, bound, cuts=(), dtype=jnp.bfloat16):
    array = jax.random.normal(stream_key, dims, jnp.float32) * scale
    if len(cuts) > 0:
        array = steps_of(stream_key, dims, cuts, -0.22, 0.18) * array
    return jnp.clip(array, min=-bound, max=bound).astype(dtype)


def setup_inputs(seed: int = 0) -> dict:
    keys = jax.random.split(jax.random.key(seed), 14)
    return {
        "tokens": scatter_about(keys[0], (TOKENS, D), 0.5, 3.0, ((0, 128),)),
        "mixer_output": scatter_about(keys[1], (TOKENS, D), 1.0, 6.0, ((0, 128),)),
        "early_norm": jnp.clip(1.0 + 0.05 * jax.random.normal(keys[2], (D,), jnp.float32), 0.75, 1.25),
        "early_gate": scatter_about(keys[3], (D, FF), D ** -0.5, 0.125, ((0, 16), (1, 4))),
        "early_value": scatter_about(keys[4], (D, FF), D ** -0.5, 0.125, ((0, 16), (1, 4))),
        "early_down": scatter_about(keys[5], (FF, D), FF ** -0.5, 0.078125, ((0, 4), (1, 16))),
        "early_post": jnp.clip(1.0 + 0.05 * jax.random.normal(keys[6], (D,), jnp.float32), 0.75, 1.25),
        "mixer_gain": jnp.clip(1.0 + 0.05 * jax.random.normal(keys[7], (D,), jnp.float32), 0.75, 1.25),
        "later_norm": jnp.clip(1.0 + 0.05 * jax.random.normal(keys[8], (D,), jnp.float32), 0.75, 1.25),
        "later_gate": scatter_about(keys[9], (D, FF), D ** -0.5, 0.125, ((0, 16), (1, 4))),
        "later_value": scatter_about(keys[10], (D, FF), D ** -0.5, 0.125, ((0, 16), (1, 4))),
        "later_down": scatter_about(keys[11], (FF, D), FF ** -0.5, 0.078125, ((0, 4), (1, 16))),
        "later_post": jnp.clip(1.0 + 0.05 * jax.random.normal(keys[12], (D,), jnp.float32), 0.75, 1.25),
    }


epsilon = 1e-06

def rms_scale(values, gain):
    values = values.astype(jnp.float32)
    scale = lax.rsqrt(lax.optimization_barrier(jnp.mean(values * values, axis=-1, keepdims=True)) + epsilon)
    return values * scale * gain

def half_branch(normed, w_gate, w_value, w_down):
    gate_sum = jnp.dot(normed, w_gate, preferred_element_type=jnp.float32)
    value_sum = jnp.dot(normed, w_value, preferred_element_type=jnp.float32)
    hidden = (jax.nn.silu(gate_sum) * value_sum).astype(jnp.bfloat16)
    return jnp.dot(hidden, w_down, preferred_element_type=jnp.float32)

def reference(tokens, mixer_output, early_norm, early_gate, early_value, early_down, early_post, mixer_gain, later_norm, later_gate, later_value, later_down, later_post):
    early_in = rms_scale(tokens, early_norm).astype(jnp.bfloat16)
    early_branch = half_branch(early_in, early_gate, early_value, early_down)
    mixed = tokens.astype(jnp.float32) + 0.5 * rms_scale(early_branch, early_post) + rms_scale(mixer_output, mixer_gain)
    mixed = mixed.astype(jnp.bfloat16)
    later_in = rms_scale(mixed, later_norm).astype(jnp.bfloat16)
    later_branch = half_branch(later_in, later_gate, later_value, later_down)
    layer_out = mixed.astype(jnp.float32) + 0.5 * rms_scale(later_branch, later_post)
    return layer_out.astype(jnp.bfloat16)
```

```python
import functools

import jax
import jax.numpy as jnp
from jax import lax
from jax.experimental import pallas as pl
from jax.experimental.pallas import tpu as pltpu
from jax.sharding import PartitionSpec as P


epsilon = 1e-06
D = 2048
PLANE = ("rep", "fs")
F32 = jnp.float32
BF16 = jnp.bfloat16


def _place(x, y, core):
    return (x // 2) * 16 + y * 4 + (x % 2) * 2 + core


def _plane_shift(dx, dy, flip):
    pairs = []
    for x in range(4):
        for y in range(4):
            for core in range(2):
                there = _place((x + dx) % 4, (y + dy) % 4, core ^ flip)
                pairs.append((_place(x, y, core), there))
    return lambda a: lax.ppermute(a, PLANE, pairs)


y_up = _plane_shift(0, 1, 0)
y_down = _plane_shift(0, -1, 0)
y_across = _plane_shift(0, 2, 0)
x_up = _plane_shift(1, 0, 0)
x_down = _plane_shift(-1, 0, 0)
to_partner = _plane_shift(0, 0, 1)


def z_shift(a, step):
    return lax.ppermute(a, "tp", [(i, (i + step) % 4) for i in range(4)])


def chips_pieces(own):
    below, above, across = y_up(own), y_down(own), y_across(own)
    column = (own, below, above, across)
    other = (x_up(own), x_up(below), x_down(above), x_down(across))
    return column + other


def rms(values, gain):
    values = values.astype(F32)
    scale = lax.rsqrt(jnp.mean(values * values, axis=-1, keepdims=True) + epsilon)
    return values * scale * gain


def _vmem(n):
    return [pl.BlockSpec(memory_space=pltpu.VMEM)] * n


def _any(n):
    return [pl.BlockSpec(memory_space=pl.ANY)] * n


_smem = pl.BlockSpec(memory_space=pltpu.SMEM)


def gate_value_kernel(place, *refs):
    tokens, weights = refs[:8], refs[8:16]
    hidden, held, sems = refs[16:]
    core = place[8]
    half = weights[0].shape[0] // 2
    copies = []
    for j in range(8):
        for part in range(2):
            side = core if part == 0 else 1 - core
            row = pl.multiple_of(place[j] * 2 * half + side * half, half)
            copies.append(
                pltpu.make_async_copy(
                    weights[j].at[pl.ds(part * half, half), :],
                    held.at[pl.ds(row, half), :],
                    sems.at[2 * j + part],
                )
            )
    for copy in copies:
        copy.start()
    for copy in copies:
        copy.wait()
    width = held.shape[1] // 2
    rows = tokens[0].shape[0]
    for m in range(4):
        block = jnp.concatenate([tokens[m][...], tokens[4 + m][...]], axis=0)
        sums = jnp.dot(block, held[...], preferred_element_type=F32)
        gate, value = sums[:, :width], sums[:, width:]
        out = gate / (1.0 + jnp.exp(-gate)) * value
        hidden[m, :, :] = out.astype(BF16)


def gate_value(place, tokens, weights):
    rows, depth = tokens[0].shape
    width = weights[0].shape[1]
    return pl.pallas_call(
        gate_value_kernel,
        out_shape=jax.ShapeDtypeStruct((4, 2 * rows, width // 2), BF16),
        in_specs=[_smem] + _vmem(8) + _any(8),
        out_specs=pl.BlockSpec(memory_space=pltpu.VMEM),
        scratch_shapes=[
            pltpu.VMEM((depth, width), BF16),
            pltpu.SemaphoreType.DMA((16,)),
        ],
        name="gate_value",
    )(place, *tokens, *weights)


def down_kernel(place, hidden, partner, *refs):
    weights = refs[:8]
    outs = refs[8:12]
    held, sems = refs[12:]
    core = place[8]
    half = weights[0].shape[0] // 2
    wide = weights[0].shape[1]
    copies = []
    for j in range(8):
        for part in range(2):
            side = core if part == 0 else 1 - core
            column = pl.multiple_of(place[j] * wide, wide)
            row = pl.multiple_of(side * half, half)
            copies.append(
                pltpu.make_async_copy(
                    weights[j].at[pl.ds(row, half), :],
                    held.at[pl.ds(part * half, half), pl.ds(column, wide)],
                    sems.at[2 * j + part],
                )
            )
    for copy in copies:
        copy.start()
    for copy in copies:
        copy.wait()
    rows = hidden.shape[1] // 2
    for m in range(4):
        swapped = jnp.concatenate([partner[m, rows:, :], partner[m, :rows, :]], axis=0)
        block = jnp.concatenate([hidden[m, :, :], swapped], axis=1)
        out = jnp.dot(block, held[...], preferred_element_type=F32)
        outs[m][...] = out.astype(outs[m].dtype)


def down(place, hidden, partner, weights):
    rows = hidden.shape[1]
    wide = 8 * weights[0].shape[1]
    return pl.pallas_call(
        down_kernel,
        out_shape=[jax.ShapeDtypeStruct((rows, wide), BF16) for _ in range(4)],
        in_specs=[_smem] + _vmem(2) + _any(8),
        out_specs=_vmem(4),
        scratch_shapes=[
            pltpu.VMEM((weights[0].shape[0], wide), BF16),
            pltpu.SemaphoreType.DMA((16,)),
        ],
        name="down",
    )(place, hidden, partner, *weights)


def _join(place, mine, theirs, joined):
    core = place[8]
    for k in range(8):
        here = pl.multiple_of((2 * k + core) * 128, 128)
        there = pl.multiple_of((2 * k + 1 - core) * 128, 128)
        joined[:, pl.ds(here, 128)] = mine[:, k * 128 : (k + 1) * 128].astype(F32)
        joined[:, pl.ds(there, 128)] = theirs[:, k * 128 : (k + 1) * 128].astype(F32)


def middle_kernel(place, mine, theirs, tokens, mixer, post, mix, norm, mixed, normed, joined):
    _join(place, mine, theirs, joined)
    branch = rms(joined[...], post[...])
    total = tokens[...].astype(F32) + 0.5 * branch + rms(mixer[...], mix[...])
    rounded = total.astype(BF16)
    mixed[...] = rounded
    normed[...] = rms(rounded, norm[...]).astype(BF16)


def last_kernel(place, mine, theirs, mixed, post, out, joined):
    _join(place, mine, theirs, joined)
    total = mixed[...].astype(F32) + 0.5 * rms(joined[...], post[...])
    out[...] = total.astype(BF16)


def gathered_tokens(normed):
    own = (normed, z_shift(normed, 1), z_shift(normed, -1), z_shift(normed, 2))
    return own + tuple(to_partner(a) for a in own)


def scattered_sum(outs):
    total = outs[0].astype(F32)
    for piece, step in ((outs[3], 2), (outs[1], -1), (outs[2], 1)):
        total = total + z_shift(piece, step).astype(F32)
    rows = total.shape[0] // 2
    theirs = to_partner(total[rows:].astype(BF16))
    return total[:rows], theirs


def gate_value_piece(core, gate, value):
    width = gate.shape[1] // 2

    def cut(side):
        return jnp.concatenate(
            [lax.dynamic_slice_in_dim(a, side * width, width, 1) for a in (gate, value)], axis=1
        )

    return jnp.concatenate([cut(core), to_partner(cut(1 - core))], axis=0)


def on_device(
    tokens,
    mixer_output,
    early_norm,
    early_gate,
    early_value,
    early_down,
    early_post,
    mixer_gain,
    later_norm,
    later_gate,
    later_value,
    later_down,
    later_post,
):
    fs = lax.axis_index("fs")
    core, side, y = fs % 2, fs // 2 % 2, fs // 4
    heights = [y, (y + 3) % 4, (y + 1) % 4, (y + 2) % 4]
    place = jnp.stack([2 * h + side for h in heights] + [2 * h + 1 - side for h in heights] + [core])
    place = place.astype(jnp.int32)

    early_wide = chips_pieces(gate_value_piece(core, early_gate, early_value))
    early_low = chips_pieces(early_down)
    later_wide = chips_pieces(gate_value_piece(core, later_gate, later_value))
    later_low = chips_pieces(later_down)

    early_in = rms(tokens, early_norm).astype(BF16)

    def half_branch(normed, wide, low):
        hidden = gate_value(place, gathered_tokens(normed), wide)
        return scattered_sum(down(place, hidden, to_partner(hidden), low))

    rows = tokens.shape[0]
    mine, theirs = half_branch(early_in, early_wide, early_low)
    shape = jax.ShapeDtypeStruct((rows, D), BF16)
    mixed, later_in = pl.pallas_call(
        middle_kernel,
        out_shape=[shape, shape],
        in_specs=[_smem] + _vmem(7),
        out_specs=_vmem(2),
        scratch_shapes=[pltpu.VMEM((rows, D), F32)],
        name="middle",
    )(place, mine, theirs, tokens, mixer_output, early_post[None], mixer_gain[None], later_norm[None])
    mine, theirs = half_branch(later_in, later_wide, later_low)
    return pl.pallas_call(
        last_kernel,
        out_shape=shape,
        in_specs=[_smem] + _vmem(4),
        out_specs=pl.BlockSpec(memory_space=pltpu.VMEM),
        scratch_shapes=[pltpu.VMEM((rows, D), F32)],
        name="last",
    )(place, mine, theirs, mixed, later_post[None])


def solution(mesh):
    placed = (
        P(("rep", "fs", "tp"), None),
        P(("rep", "fs", "tp"), None),
        P(),
        P("fs", "tp"),
        P("fs", "tp"),
        P("tp", "fs"),
        P(),
        P(),
        P(),
        P("fs", "tp"),
        P("fs", "tp"),
        P("tp", "fs"),
        P(),
    )
    return jax.shard_map(
        on_device,
        mesh=mesh,
        in_specs=placed,
        out_specs=P(("rep", "fs", "tp"), None),
        check_vma=False,
    )
```

```python
import jax
import jax.numpy as jnp
from jax import lax
from jax.experimental import pallas as pl
from jax.experimental.pallas import tpu as pltpu
from jax.sharding import PartitionSpec as P


epsilon = 1e-06
PLANE = ("rep", "fs")
F32 = jnp.float32
BF16 = jnp.bfloat16


def _place(x, y, core):
    return (x // 2) * 16 + y * 4 + (x % 2) * 2 + core


def _plane_shift(dx, dy, flip):
    pairs = []
    for x in range(4):
        for y in range(4):
            for core in range(2):
                there = _place((x + dx) % 4, (y + dy) % 4, core ^ flip)
                pairs.append((_place(x, y, core), there))
    return lambda a: lax.ppermute(a, PLANE, pairs)


y_up = _plane_shift(0, 1, 0)
y_down = _plane_shift(0, -1, 0)
y_across = _plane_shift(0, 2, 0)
x_up = _plane_shift(1, 0, 0)
x_down = _plane_shift(-1, 0, 0)
to_partner = _plane_shift(0, 0, 1)


def z_shift(step):
    return lambda a: lax.ppermute(a, "tp", [(i, (i + step) % 4) for i in range(4)])


def all_pieces(own, ways):
    below = y_up(own)
    above = y_down(own)
    across = y_across(own)
    pieces = [own, below, above, across]
    for i, way in enumerate(ways):
        pieces.append((x_up if way == "+" else x_down)(pieces[i]))
    out = []
    for piece in pieces:
        out += [piece, to_partner(piece)]
    return out


def rms(values, gain):
    values = values.astype(F32)
    scale = lax.rsqrt(jnp.mean(values * values, axis=-1, keepdims=True) + epsilon)
    return values * scale * gain


def _vmem(n):
    return [pl.BlockSpec(memory_space=pltpu.VMEM)] * n


_smem = pl.BlockSpec(memory_space=pltpu.SMEM)
CHIPS = 4
COLUMNS = 256
GATE_VALUE_LIMIT = 18 << 20
DOWN_LIMIT = 6 << 20
SMALL_LIMIT = 4 << 20


def gate_value_kernel(place, *refs):
    count = len(refs) - 19
    tokens, weights, (hidden, gates, values) = refs[:count], refs[count:-3], refs[-3:]
    core = place[8]
    half = weights[0].shape[0] // 2
    width = weights[0].shape[1]
    for start in range(0, 8, CHIPS):
        sides = [(j, part) for j in range(start, start + CHIPS) for part in range(2)]
        blocks = []
        for j, part in sides:
            side = core if part == 0 else 1 - core
            at = pl.ds(pl.multiple_of((place[j] * 2 + side) * half, half), half)
            blocks.append(jnp.concatenate([t[:, at] for t in tokens], axis=0))
        block = jnp.concatenate(blocks, axis=1)

        def columns(i, carry, start=start, sides=sides, block=block):
            at = pl.ds(pl.multiple_of(i * COLUMNS, COLUMNS), COLUMNS)
            gate = jnp.concatenate([weights[2 * j + part][:half, at] for j, part in sides], axis=0)
            value = jnp.concatenate([weights[2 * j + part][half:, at] for j, part in sides], axis=0)
            gate = jnp.dot(block, gate, preferred_element_type=F32)
            value = jnp.dot(block, value, preferred_element_type=F32)
            if start > 0:
                gate = gate + gates[:, at]
                value = value + values[:, at]
            if start + CHIPS < 8:
                gates[:, at] = gate
                values[:, at] = value
            else:
                hidden[:, at] = (gate / (1.0 + jnp.exp(-gate)) * value).astype(BF16)
            return carry

        lax.fori_loop(0, width // COLUMNS, columns, 0)


def gate_value(place, tokens, weights):
    rows = len(tokens) * tokens[0].shape[0]
    width = weights[0].shape[1]
    return pl.pallas_call(
        gate_value_kernel,
        out_shape=jax.ShapeDtypeStruct((rows, width), BF16),
        in_specs=[_smem] + _vmem(len(tokens) + 16),
        out_specs=pl.BlockSpec(memory_space=pltpu.VMEM),
        scratch_shapes=[pltpu.VMEM((rows, width), F32)] * 2,
        compiler_params=pltpu.CompilerParams(vmem_limit_bytes=GATE_VALUE_LIMIT),
        cost_estimate=pl.CostEstimate(flops=8 * rows * 2048 * width, bytes_accessed=0, transcendentals=0),
    )(place, *tokens, *weights)


def down_kernel(place, hidden, *refs):
    weights, outs = refs[:16], refs[16:]
    core = place[8]
    rows = hidden.shape[0] // len(outs)
    wide = weights[0].shape[1]
    for j in range(8):
        pair = jnp.concatenate([weights[2 * j][...], weights[2 * j + 1][...]], axis=1)
        sums = jnp.dot(hidden[...], pair, preferred_element_type=F32)
        for part in range(2):
            side = core if part == 0 else 1 - core
            at = pl.ds(pl.multiple_of((place[j] * 2 + side) * wide, wide), wide)
            mine = sums[:, part * wide : (part + 1) * wide]
            for i, out in enumerate(outs):
                out[:, at] = mine[i * rows : (i + 1) * rows].astype(out.dtype)


def down(place, hidden, weights, types):
    rows = hidden.shape[0] // len(types)
    wide = 16 * weights[0].shape[1]
    return pl.pallas_call(
        down_kernel,
        out_shape=[jax.ShapeDtypeStruct((rows, wide), t) for t in types],
        in_specs=[_smem] + _vmem(17),
        out_specs=_vmem(len(types)),
        compiler_params=pltpu.CompilerParams(vmem_limit_bytes=DOWN_LIMIT),
        cost_estimate=pl.CostEstimate(
            flops=2 * hidden.shape[0] * hidden.shape[1] * wide, bytes_accessed=0, transcendentals=0
        ),
    )(place, hidden, *weights)


def early_norm_kernel(tokens, norm, normed):
    normed[...] = rms(tokens[...], norm[...]).astype(BF16)


def _total(parts):
    total = parts[0][...]
    for part in parts[1:]:
        total = total + part[...].astype(F32)
    return total


def middle_kernel(p0, p1, p2, p3, tokens, mixer, post, mix, norm, mixed, normed):
    branch = rms(_total((p0, p1, p2, p3)), post[...])
    total = tokens[...].astype(F32) + 0.5 * branch + rms(mixer[...], mix[...])
    rounded = total.astype(BF16)
    mixed[...] = rounded
    normed[...] = rms(rounded, norm[...]).astype(BF16)


def last_kernel(p0, p1, p2, p3, mixed, post, out):
    branch = rms(_total((p0, p1, p2, p3)), post[...])
    out[...] = (mixed[...].astype(F32) + 0.5 * branch).astype(BF16)


def simple(kernel, shape, outs, *args):
    shapes = [jax.ShapeDtypeStruct(shape, BF16)] * outs
    return pl.pallas_call(
        kernel,
        out_shape=shapes,
        in_specs=_vmem(len(args)),
        out_specs=_vmem(outs),
        compiler_params=pltpu.CompilerParams(vmem_limit_bytes=SMALL_LIMIT),
    )(*args)


def on_device(
    tokens,
    mixer_output,
    early_norm,
    early_gate,
    early_value,
    early_down,
    early_post,
    mixer_gain,
    later_norm,
    later_gate,
    later_value,
    later_down,
    later_post,
):
    fs = lax.axis_index("fs")
    core, side, y = fs % 2, fs // 2 % 2, fs // 4
    heights = [y, (y + 3) % 4, (y + 1) % 4, (y + 2) % 4]
    place = [2 * h + side for h in heights] + [2 * h + 1 - side for h in heights] + [core]
    place = jnp.stack(place).astype(jnp.int32)

    early_wide = all_pieces(jnp.concatenate([early_gate, early_value], axis=0), "++--")
    early_low = all_pieces(early_down, "-++-")
    later_wide = all_pieces(jnp.concatenate([later_gate, later_value], axis=0), "++--")
    later_low = all_pieces(later_down, "-++-")
    shape = tokens.shape

    def gathered(normed):
        across = z_shift(2)(normed)
        under = z_shift(1)(normed)
        over = z_shift(-1)(normed)
        return across, normed, under, over

    def scattered(across, own, under, over):
        return (own, z_shift(2)(across), z_shift(1)(over), z_shift(-1)(under))

    (early_in,) = simple(early_norm_kernel, shape, 1, tokens, early_norm[None])
    hidden = gate_value(place, gathered(early_in), early_wide)
    parts = scattered(*down(place, hidden, early_low, (BF16, F32, BF16, BF16)))
    gains = (early_post[None], mixer_gain[None], later_norm[None])
    mixed, later_in = simple(middle_kernel, shape, 2, *parts, tokens, mixer_output, *gains)
    rows = gathered(later_in)
    hidden = gate_value(place, rows[:2], later_wide)
    first = down(place, hidden, later_low, (BF16, F32))
    hidden = gate_value(place, rows[2:], later_wide)
    second = down(place, hidden, later_low, (BF16, BF16))
    parts = scattered(*first, *second)
    (out,) = simple(last_kernel, shape, 1, *parts, mixed, later_post[None])
    return out


def solution(mesh):
    placed = (
        P(("rep", "fs", "tp"), None),
        P(("rep", "fs", "tp"), None),
        P(),
        P("fs", "tp"),
        P("fs", "tp"),
        P("tp", "fs"),
        P(),
        P(),
        P(),
        P("fs", "tp"),
        P("fs", "tp"),
        P("tp", "fs"),
        P(),
    )
    return jax.shard_map(
        on_device,
        mesh=mesh,
        in_specs=placed,
        out_specs=P(("rep", "fs", "tp"), None),
        check_vma=False,
    )
```

```python
import functools

import jax
import jax.numpy as jnp
from jax import lax
from jax.experimental import pallas as pl
from jax.experimental.pallas import tpu as pltpu
from jax.sharding import PartitionSpec as P


epsilon = 1e-06
PLANE = ("rep", "fs")
F32 = jnp.float32
BF16 = jnp.bfloat16


def _place(x, y, core):
    return (x // 2) * 16 + y * 4 + (x % 2) * 2 + core


def _plane_shift(dx, dy, flip):
    pairs = []
    for x in range(4):
        for y in range(4):
            for core in range(2):
                there = _place((x + dx) % 4, (y + dy) % 4, core ^ flip)
                pairs.append((_place(x, y, core), there))
    return lambda a: lax.ppermute(a, PLANE, pairs)


y_up = _plane_shift(0, 1, 0)
y_down = _plane_shift(0, -1, 0)
y_across = _plane_shift(0, 2, 0)
x_up = _plane_shift(1, 0, 0)
x_down = _plane_shift(-1, 0, 0)
to_partner = _plane_shift(0, 0, 1)


def z_shift(step):
    return lambda a: lax.ppermute(a, "tp", [(i, (i + step) % 4) for i in range(4)])


def all_pieces(own, ways):
    below = y_up(own)
    above = y_down(own)
    across = y_across(own)
    pieces = [own, below, above, across]
    for i, way in enumerate(ways):
        pieces.append((x_up if way == "+" else x_down)(pieces[i]))
    out = []
    for piece in pieces:
        out += [piece, to_partner(piece)]
    return out


def rms(values, gain):
    values = values.astype(F32)
    scale = lax.rsqrt(jnp.mean(values * values, axis=-1, keepdims=True) + epsilon)
    return values * scale * gain


def _vmem(n):
    return [pl.BlockSpec(memory_space=pltpu.VMEM)] * n


def places():
    fs = lax.axis_index("fs")
    core, side, y = lax.rem(fs, 2), lax.rem(lax.div(fs, 2), 2), lax.div(fs, 4)
    heights = [lax.rem(y + step, 4) for step in (0, 3, 1, 2)]
    return [2 * h + side for h in heights] + [2 * h + 1 - side for h in heights], core


def in_vmem(arrays):
    return tuple(pltpu.with_memory_space_constraint(a, pltpu.VMEM) for a in arrays)


CHIPS = 4
COLUMNS = 256
DOWN_LIMIT = 6 << 20
SMALL_LIMIT = 4 << 20


def gate_value_kernel(chips, count, begun, ended, *refs):
    tokens, refs = refs[:count], refs[count:]
    weights, refs = refs[: 2 * len(chips)], refs[2 * len(chips) :]
    before, refs = (refs[:2], refs[2:]) if begun else ((), refs)
    hidden, sums = (refs[0], refs[1:]) if ended else (None, refs)
    place, core = places()
    half = weights[0].shape[0] // 2
    width = weights[0].shape[1]
    for start in range(0, len(chips), CHIPS):
        sides = [(i, part) for i in range(start, start + CHIPS) for part in range(2)]
        blocks = []
        for i, part in sides:
            side = core if part == 0 else 1 - core
            at = pl.ds(pl.multiple_of((place[chips[i]] * 2 + side) * half, half), half)
            blocks.append(jnp.concatenate([t[:, at] for t in tokens], axis=0))
        block = jnp.concatenate(blocks, axis=1)
        held = sums if start > 0 else before
        final = ended and start + CHIPS == len(chips)

        def columns(k, carry, sides=sides, block=block, held=held, final=final):
            at = pl.ds(pl.multiple_of(k * COLUMNS, COLUMNS), COLUMNS)
            gate = jnp.concatenate([weights[2 * i + part][:half, at] for i, part in sides], axis=0)
            value = jnp.concatenate([weights[2 * i + part][half:, at] for i, part in sides], axis=0)
            gate = jnp.dot(block, gate, preferred_element_type=F32)
            value = jnp.dot(block, value, preferred_element_type=F32)
            if held:
                gate = gate + held[0][:, at]
                value = value + held[1][:, at]
            if final:
                hidden[:, at] = (gate / (1.0 + jnp.exp(-gate)) * value).astype(BF16)
            else:
                sums[0][:, at] = gate
                sums[1][:, at] = value
            return carry

        lax.fori_loop(0, width // COLUMNS, columns, 0)


def gate_value(tokens, weights, chips=tuple(range(8)), before=(), ended=True, limit=0):
    rows = len(tokens) * tokens[0].shape[0]
    weights = [weights[2 * j + part] for j in chips for part in range(2)]
    width = weights[0].shape[1]
    partial = [jax.ShapeDtypeStruct((rows, width), F32)] * 2
    out = [jax.ShapeDtypeStruct((rows, width), BF16)] if ended else partial
    held = ended and len(chips) > CHIPS
    args = (*in_vmem(tokens), *in_vmem(weights), *in_vmem(before))
    return pl.pallas_call(
        functools.partial(gate_value_kernel, chips, len(tokens), bool(before), ended),
        out_shape=out,
        in_specs=_vmem(len(args)),
        out_specs=_vmem(len(out)),
        scratch_shapes=[pltpu.VMEM((rows, width), F32)] * (2 if held else 0),
        compiler_params=pltpu.CompilerParams(vmem_limit_bytes=limit << 20),
        cost_estimate=pl.CostEstimate(
            flops=8 * rows * 128 * len(weights) * width, bytes_accessed=0, transcendentals=0
        ),
    )(*args)


def down_kernel(hidden, *refs):
    weights, outs = refs[:16], refs[16:]
    place, core = places()
    rows = hidden.shape[0] // len(outs)
    wide = weights[0].shape[1]
    for j in range(8):
        pair = jnp.concatenate([weights[2 * j][...], weights[2 * j + 1][...]], axis=1)
        sums = jnp.dot(hidden[...], pair, preferred_element_type=F32)
        for part in range(2):
            side = core if part == 0 else 1 - core
            at = pl.ds(pl.multiple_of((place[j] * 2 + side) * wide, wide), wide)
            mine = sums[:, part * wide : (part + 1) * wide]
            for i, out in enumerate(outs):
                out[:, at] = mine[i * rows : (i + 1) * rows].astype(out.dtype)


def down(hidden, weights, types):
    rows = hidden.shape[0] // len(types)
    wide = 16 * weights[0].shape[1]
    return pl.pallas_call(
        down_kernel,
        out_shape=[jax.ShapeDtypeStruct((rows, wide), t) for t in types],
        in_specs=_vmem(17),
        out_specs=_vmem(len(types)),
        compiler_params=pltpu.CompilerParams(vmem_limit_bytes=DOWN_LIMIT),
        cost_estimate=pl.CostEstimate(
            flops=2 * hidden.shape[0] * hidden.shape[1] * wide, bytes_accessed=0, transcendentals=0
        ),
    )(*in_vmem((hidden, *weights)))


def early_norm_kernel(tokens, norm, normed):
    normed[...] = rms(tokens[...], norm[...]).astype(BF16)


def _total(parts):
    total = parts[0][...]
    for part in parts[1:]:
        total = total + part[...].astype(F32)
    return total


def middle_kernel(p0, p1, p2, p3, tokens, mixer, post, mix, norm, mixed, normed):
    branch = rms(_total((p0, p1, p2, p3)), post[...])
    total = tokens[...].astype(F32) + 0.5 * branch + rms(mixer[...], mix[...])
    rounded = total.astype(BF16)
    mixed[...] = rounded
    normed[...] = rms(rounded, norm[...]).astype(BF16)


def last_kernel(p0, p1, p2, p3, mixed, post, out):
    branch = rms(_total((p0, p1, p2, p3)), post[...])
    out[...] = (mixed[...].astype(F32) + 0.5 * branch).astype(BF16)


def simple(kernel, shape, outs, *args):
    shapes = [jax.ShapeDtypeStruct(shape, BF16)] * outs
    return pl.pallas_call(
        kernel,
        out_shape=shapes,
        in_specs=_vmem(len(args)),
        out_specs=_vmem(outs),
        compiler_params=pltpu.CompilerParams(vmem_limit_bytes=SMALL_LIMIT),
    )(*args)


def join_kernel(gate, value, joined, sems):
    rows = gate.shape[0]
    first = pltpu.make_async_copy(gate, joined.at[pl.ds(0, rows), :], sems.at[0])
    second = pltpu.make_async_copy(value, joined.at[pl.ds(rows, rows), :], sems.at[1])
    first.start()
    second.start()
    first.wait()
    second.wait()


def join(gate, value):
    rows, width = gate.shape
    return pl.pallas_call(
        join_kernel,
        out_shape=jax.ShapeDtypeStruct((2 * rows, width), BF16),
        in_specs=[pl.BlockSpec(memory_space=pltpu.HBM)] * 2,
        out_specs=pl.BlockSpec(memory_space=pltpu.VMEM),
        scratch_shapes=[pltpu.SemaphoreType.DMA((2,))],
        compiler_params=pltpu.CompilerParams(vmem_limit_bytes=SMALL_LIMIT),
    )(*(pltpu.with_memory_space_constraint(a, pltpu.HBM) for a in (gate, value)))


def on_device(
    tokens,
    mixer_output,
    early_norm,
    early_gate,
    early_value,
    early_down,
    early_post,
    mixer_gain,
    later_norm,
    later_gate,
    later_value,
    later_down,
    later_post,
):
    early_wide = all_pieces(join(early_gate, early_value), "++--")
    early_low = all_pieces(early_down, "-++-")
    later_wide = all_pieces(join(later_gate, later_value), "++--")
    later_low = all_pieces(later_down, "++-+")
    shape = tokens.shape

    def gathered(normed):
        across = z_shift(2)(normed)
        under = z_shift(1)(normed)
        over = z_shift(-1)(normed)
        return across, normed, under, over

    def scattered(across, own, under, over):
        return (own, z_shift(2)(across), z_shift(1)(over), z_shift(-1)(under))

    (early_in,) = simple(early_norm_kernel, shape, 1, tokens, early_norm[None])
    rows = gathered(early_in)
    sums = gate_value(rows, early_wide, (0, 3, 4, 7), ended=False, limit=18)
    (hidden,) = gate_value(rows, early_wide, (1, 2, 5, 6), sums, limit=18)
    parts = scattered(*down(hidden, early_low, (BF16, F32, BF16, BF16)))
    gains = (early_post[None], mixer_gain[None], later_norm[None])
    mixed, later_in = simple(middle_kernel, shape, 2, *parts, tokens, mixer_output, *gains)
    rows = gathered(later_in)
    (hidden,) = gate_value(rows[:2], later_wide, limit=8)
    first = down(hidden, later_low, (BF16, F32))
    (hidden,) = gate_value(rows[2:], later_wide, limit=8)
    second = down(hidden, later_low, (BF16, BF16))
    parts = scattered(*first, *second)
    (out,) = simple(last_kernel, shape, 1, *parts, mixed, later_post[None])
    return out


def solution(mesh):
    placed = (
        P(("rep", "fs", "tp"), None),
        P(("rep", "fs", "tp"), None),
        P(),
        P("fs", "tp"),
        P("fs", "tp"),
        P("tp", "fs"),
        P(),
        P(),
        P(),
        P("fs", "tp"),
        P("fs", "tp"),
        P("tp", "fs"),
        P(),
    )
    return jax.shard_map(
        on_device,
        mesh=mesh,
        in_specs=placed,
        out_specs=P(("rep", "fs", "tp"), None),
        check_vma=False,
    )
```

```python
import functools

import jax
import jax.numpy as jnp
from jax import lax
from jax.experimental import pallas as pl
from jax.experimental.pallas import tpu as pltpu
from jax.sharding import PartitionSpec as P


epsilon = 1e-06
PLANE = ("rep", "fs")
F32 = jnp.float32
BF16 = jnp.bfloat16


def _place(x, y, core):
    return (x // 2) * 16 + y * 4 + (x % 2) * 2 + core


def _plane_shift(dx, dy, flip):
    pairs = []
    for x in range(4):
        for y in range(4):
            for core in range(2):
                there = _place((x + dx) % 4, (y + dy) % 4, core ^ flip)
                pairs.append((_place(x, y, core), there))
    return lambda a: lax.ppermute(a, PLANE, pairs)


y_up = _plane_shift(0, 1, 0)
y_down = _plane_shift(0, -1, 0)
y_across = _plane_shift(0, 2, 0)
x_up = _plane_shift(1, 0, 0)
x_down = _plane_shift(-1, 0, 0)
to_partner = _plane_shift(0, 0, 1)


def z_shift(step):
    return lambda a: lax.ppermute(a, "tp", [(i, (i + step) % 4) for i in range(4)])


def all_pieces(own, ways, halved=False, turned=False):
    below = y_up(own)
    above = y_down(own)
    across = y_across(own)
    pieces = [own, below, above, across]
    for i, way in enumerate(ways):
        send, piece = x_up if way == "+" else x_down, pieces[i]
        if turned and i in (1, 2):
            send, piece = (y_up, y_down)[i - 1], pieces[4]
        pieces.append(send(piece))
    out = []
    for piece in pieces:
        out += [piece, to_partner(piece)]
    if halved:
        gate, value = halve(across)
        last = (x_up(gate), x_down(value))
        out += [last, tuple(to_partner(a) for a in last)]
    return out


def halve_kernel(whole, low, high):
    rows = low.shape[0]
    low[...] = whole[:rows, :]
    high[...] = whole[rows:, :]


def halve(whole):
    half = (whole.shape[0] // 2, whole.shape[1])
    return simple(halve_kernel, half, 2, whole)


def rms(values, gain):
    values = values.astype(F32)
    scale = lax.rsqrt(jnp.mean(values * values, axis=-1, keepdims=True) + epsilon)
    return values * scale * gain


def _vmem(n):
    return [pl.BlockSpec(memory_space=pltpu.VMEM)] * n


def places():
    fs = lax.axis_index("fs")
    core, side, y = lax.rem(fs, 2), lax.rem(lax.div(fs, 2), 2), lax.div(fs, 4)
    heights = [lax.rem(y + step, 4) for step in (0, 3, 1, 2)]
    return [2 * h + side for h in heights] + [2 * h + 1 - side for h in heights], core


def in_vmem(arrays):
    return tuple(pltpu.with_memory_space_constraint(a, pltpu.VMEM) for a in arrays)


CHIPS = 4
COLUMNS = 256
DOWN_LIMIT = 6 << 20
SMALL_LIMIT = 4 << 20


def gate_value_kernel(chips, count, split, begun, ended, *refs):
    tokens, refs = refs[:count], refs[count:]
    weights = []
    for is_split in split:
        taken = 2 if is_split else 1
        weights.append(refs[:taken])
        refs = refs[taken:]
    before, refs = (refs[:2], refs[2:]) if begun else ((), refs)
    hidden, sums = (refs[0], refs[1:]) if ended else (None, refs)
    place, core = places()
    half = weights[0][0].shape[0] // 2
    width = weights[0][0].shape[1]

    def rows(i, which, at):
        if len(weights[i]) == 2:
            return weights[i][which][:, at]
        return weights[i][0][which * half : (which + 1) * half, at]

    for start in range(0, len(chips), CHIPS):
        sides = [(i, part) for i in range(start, start + CHIPS) for part in range(2)]
        blocks = []
        for i, part in sides:
            side = core if part == 0 else 1 - core
            at = pl.ds(pl.multiple_of((place[chips[i]] * 2 + side) * half, half), half)
            blocks.append(jnp.concatenate([t[:, at] for t in tokens], axis=0))
        block = jnp.concatenate(blocks, axis=1)
        held = sums if start > 0 else before
        final = ended and start + CHIPS == len(chips)

        def columns(k, carry, sides=sides, block=block, held=held, final=final):
            at = pl.ds(pl.multiple_of(k * COLUMNS, COLUMNS), COLUMNS)
            gate = jnp.concatenate([rows(2 * i + part, 0, at) for i, part in sides], axis=0)
            value = jnp.concatenate([rows(2 * i + part, 1, at) for i, part in sides], axis=0)
            gate = jnp.dot(block, gate, preferred_element_type=F32)
            value = jnp.dot(block, value, preferred_element_type=F32)
            if held:
                gate = gate + held[0][:, at]
                value = value + held[1][:, at]
            if final:
                hidden[:, at] = (gate / (1.0 + jnp.exp(-gate)) * value).astype(BF16)
            else:
                sums[0][:, at] = gate
                sums[1][:, at] = value
            return carry

        lax.fori_loop(0, width // COLUMNS, columns, 0)


def gate_value(tokens, weights, chips=tuple(range(8)), before=(), ended=True, limit=0):
    rows = len(tokens) * tokens[0].shape[0]
    weights = [weights[2 * j + part] for j in chips for part in range(2)]
    split = tuple(isinstance(w, tuple) for w in weights)
    flat = [a for w in weights for a in (w if isinstance(w, tuple) else (w,))]
    width = flat[0].shape[1]
    partial = [jax.ShapeDtypeStruct((rows, width), F32)] * 2
    out = [jax.ShapeDtypeStruct((rows, width), BF16)] if ended else partial
    held = ended and len(chips) > CHIPS
    args = (*in_vmem(tokens), *in_vmem(flat), *in_vmem(before))
    return pl.pallas_call(
        functools.partial(gate_value_kernel, chips, len(tokens), split, bool(before), ended),
        out_shape=out,
        in_specs=_vmem(len(args)),
        out_specs=_vmem(len(out)),
        scratch_shapes=[pltpu.VMEM((rows, width), F32)] * (2 if held else 0),
        compiler_params=pltpu.CompilerParams(vmem_limit_bytes=limit << 20),
        cost_estimate=pl.CostEstimate(
            flops=8 * rows * 128 * len(weights) * width, bytes_accessed=0, transcendentals=0
        ),
    )(*args)


def down_kernel(start, counts, split, hidden, *refs):
    weights = []
    for is_split in split:
        taken = 2 if is_split else 1
        weights.append(refs[:taken])
        refs = refs[taken:]
    added, outs = refs[: -len(counts)], refs[-len(counts) :]
    place, core = places()
    wide = weights[0][0].shape[1]
    block = hidden[start : start + sum(counts), :]
    for j in range(8):
        pair = [jnp.concatenate([w[...] for w in weights[2 * j + part]], axis=0) for part in range(2)]
        pair = jnp.concatenate(pair, axis=1)
        sums = jnp.dot(block, pair, preferred_element_type=F32)
        for part in range(2):
            side = core if part == 0 else 1 - core
            at = pl.ds(pl.multiple_of((place[j] * 2 + side) * wide, wide), wide)
            mine = sums[:, part * wide : (part + 1) * wide]
            row = 0
            for out, count in zip(outs, counts):
                rows = mine[row : row + count]
                if added:
                    low, high = rows[: count // 2], rows[count // 2 :]
                    if row == 0:
                        high = high + added[1][:, at].astype(F32)
                    else:
                        low = low + added[0][:, at].astype(F32)
                    rows = jnp.concatenate([low, high], axis=0)
                out[:, at] = rows.astype(out.dtype)
                row += count


def down(hidden, weights, start, outs, added=()):
    counts = tuple(rows for rows, _ in outs)
    wide = 16 * weights[0].shape[1]
    split = tuple(isinstance(w, tuple) for w in weights)
    flat = [a for w in weights for a in (w if isinstance(w, tuple) else (w,))]
    args = in_vmem((hidden, *flat, *added))
    return pl.pallas_call(
        functools.partial(down_kernel, start, counts, split),
        out_shape=[jax.ShapeDtypeStruct((rows, wide), t) for rows, t in outs],
        in_specs=_vmem(len(args)),
        out_specs=_vmem(len(outs)),
        compiler_params=pltpu.CompilerParams(vmem_limit_bytes=DOWN_LIMIT),
        cost_estimate=pl.CostEstimate(
            flops=2 * sum(counts) * hidden.shape[1] * wide, bytes_accessed=0, transcendentals=0
        ),
    )(*args)


def early_norm_kernel(tokens, norm, normed):
    normed[...] = rms(tokens[...], norm[...]).astype(BF16)


def add_kernel(over_low, under_high, low, high, over_out, under_out):
    over_out[...] = (over_low[...] + low[...].astype(F32)).astype(BF16)
    under_out[...] = (under_high[...] + high[...].astype(F32)).astype(BF16)


def _total(parts):
    total = parts[0][...]
    for part in parts[1:]:
        total = total + part.astype(F32)
    return total


def middle_kernel(own, p_low, p_high, m_low, m_high, tokens, mixer, post, mix, norm, mixed, normed):
    below = jnp.concatenate([p_low[...], p_high[...]], axis=0)
    above = jnp.concatenate([m_low[...], m_high[...]], axis=0)
    branch = rms(_total((own, below, above)), post[...])
    total = tokens[...].astype(F32) + 0.5 * branch + rms(mixer[...], mix[...])
    rounded = total.astype(BF16)
    mixed[...] = rounded
    normed[...] = rms(rounded, norm[...]).astype(BF16)


def last_kernel(p0, p1, p2, mixed, post, out):
    branch = rms(_total((p0, p1[...], p2[...])), post[...])
    out[...] = (mixed[...].astype(F32) + 0.5 * branch).astype(BF16)


def simple(kernel, shape, outs, *args):
    shapes = [jax.ShapeDtypeStruct(shape, BF16)] * outs
    return pl.pallas_call(
        kernel,
        out_shape=shapes,
        in_specs=_vmem(len(args)),
        out_specs=_vmem(outs),
        compiler_params=pltpu.CompilerParams(vmem_limit_bytes=SMALL_LIMIT),
    )(*args)


def join_kernel(gate, value, joined, sems):
    rows = gate.shape[0]
    first = pltpu.make_async_copy(gate, joined.at[pl.ds(0, rows), :], sems.at[0])
    second = pltpu.make_async_copy(value, joined.at[pl.ds(rows, rows), :], sems.at[1])
    first.start()
    second.start()
    first.wait()
    second.wait()


def join(gate, value):
    rows, width = gate.shape
    return pl.pallas_call(
        join_kernel,
        out_shape=jax.ShapeDtypeStruct((2 * rows, width), BF16),
        in_specs=[pl.BlockSpec(memory_space=pltpu.HBM)] * 2,
        out_specs=pl.BlockSpec(memory_space=pltpu.VMEM),
        scratch_shapes=[pltpu.SemaphoreType.DMA((2,))],
        compiler_params=pltpu.CompilerParams(vmem_limit_bytes=SMALL_LIMIT),
    )(*(pltpu.with_memory_space_constraint(a, pltpu.HBM) for a in (gate, value)))


def on_device(
    tokens,
    mixer_output,
    early_norm,
    early_gate,
    early_value,
    early_down,
    early_post,
    mixer_gain,
    later_norm,
    later_gate,
    later_value,
    later_down,
    later_post,
):
    early_wide = all_pieces(join(early_gate, early_value), "++--")
    early_low = all_pieces(early_down, "-++-", turned=True)
    later_wide = all_pieces(join(later_gate, later_value), "++-", halved=True)
    later_low = all_pieces(later_down, "-+++", turned=True)
    shape = tokens.shape

    def gathered(normed):
        across = z_shift(2)(normed)
        under = z_shift(1)(normed)
        over = z_shift(-1)(normed)
        return across, normed, under, over

    half, whole = shape[0] // 2, shape[0]
    far = ((half, BF16), (half, BF16), (whole, F32))
    near = ((whole, BF16), (whole, BF16))

    def passed_on(low, high):
        return z_shift(1)(low), z_shift(-1)(high)

    def returned(under, over):
        return z_shift(1)(over), z_shift(-1)(under)

    (early_in,) = simple(early_norm_kernel, shape, 1, tokens, early_norm[None])
    rows = gathered(early_in)
    sums = gate_value(rows, early_wide, (0, 3, 4, 7), ended=False, limit=18)
    (hidden,) = gate_value(rows, early_wide, (1, 2, 5, 6), sums, limit=18)
    low, high, own = down(hidden, early_low, 0, far)
    added = passed_on(low, high)
    quarter = ((half, BF16), (half, F32), (half, F32), (half, BF16))
    under_low, under_high, over_low, over_high = down(hidden, early_low, 2 * whole, quarter)
    p_high, m_low = z_shift(1)(over_high), z_shift(-1)(under_low)
    over_low, under_high = simple(add_kernel, (half, shape[1]), 2, over_low, under_high, *added)
    p_low, m_high = z_shift(1)(over_low), z_shift(-1)(under_high)
    parts = (own, p_low, p_high, m_low, m_high)
    gains = (early_post[None], mixer_gain[None], later_norm[None])
    mixed, later_in = simple(middle_kernel, shape, 2, *parts, tokens, mixer_output, *gains)
    rows = gathered(later_in)
    (hidden,) = gate_value(rows[:2], later_wide, limit=8)
    low, high, own = down(hidden, later_low, 0, far)
    added = passed_on(low, high)
    (hidden,) = gate_value(rows[2:], later_wide, limit=8)
    near_sums = down(hidden, later_low, 0, near, added)
    parts = (own, *returned(*near_sums))
    (out,) = simple(last_kernel, shape, 1, *parts, mixed, later_post[None])
    return out


def solution(mesh):
    placed = (
        P(("rep", "fs", "tp"), None),
        P(("rep", "fs", "tp"), None),
        P(),
        P("fs", "tp"),
        P("fs", "tp"),
        P("tp", "fs"),
        P(),
        P(),
        P(),
        P("fs", "tp"),
        P("fs", "tp"),
        P("tp", "fs"),
        P(),
    )
    return jax.shard_map(
        on_device,
        mesh=mesh,
        in_specs=placed,
        out_specs=P(("rep", "fs", "tp"), None),
        check_vma=False,
    )
```

```python
import functools

import jax
import jax.numpy as jnp
from jax import lax
from jax.experimental import pallas as pl
from jax.experimental.pallas import tpu as pltpu
from jax.sharding import PartitionSpec as P


epsilon = 1e-06
PLANE = ("rep", "fs")
F32 = jnp.float32
BF16 = jnp.bfloat16


def _place(x, y, core):
    return (x // 2) * 16 + y * 4 + (x % 2) * 2 + core


def _plane_shift(dx, dy, flip):
    pairs = []
    for x in range(4):
        for y in range(4):
            for core in range(2):
                there = _place((x + dx) % 4, (y + dy) % 4, core ^ flip)
                pairs.append((_place(x, y, core), there))
    return lambda a: lax.ppermute(a, PLANE, pairs)


y_up = _plane_shift(0, 1, 0)
y_down = _plane_shift(0, -1, 0)
y_across = _plane_shift(0, 2, 0)
x_up = _plane_shift(1, 0, 0)
x_down = _plane_shift(-1, 0, 0)
to_partner = _plane_shift(0, 0, 1)


def z_shift(step):
    return lambda a: lax.ppermute(a, "tp", [(i, (i + step) % 4) for i in range(4)])


def all_pieces(own, ways, halved=False, turned=False):
    below = y_up(own)
    above = y_down(own)
    across = y_across(own)
    pieces = [own, below, above, across]
    for i, way in enumerate(ways):
        send, piece = x_up if way == "+" else x_down, pieces[i]
        if turned and i in (1, 2):
            send, piece = (y_up, y_down)[i - 1], pieces[4]
        pieces.append(send(piece))
    out = []
    for piece in pieces:
        out += [piece, to_partner(piece)]
    if halved:
        gate, value = halve(across)
        last = (x_up(gate), x_down(value))
        out += [last, tuple(to_partner(a) for a in last)]
    return out


def halve_kernel(whole, low, high):
    rows = low.shape[0]
    low[...] = whole[:rows, :]
    high[...] = whole[rows:, :]


def halve(whole):
    half = (whole.shape[0] // 2, whole.shape[1])
    return simple(halve_kernel, half, 2, whole)


def rms(values, gain):
    values = values.astype(F32)
    scale = lax.rsqrt(jnp.mean(values * values, axis=-1, keepdims=True) + epsilon)
    return values * scale * gain


def _vmem(n):
    return [pl.BlockSpec(memory_space=pltpu.VMEM)] * n


def places():
    fs = lax.axis_index("fs")
    core, side, y = lax.rem(fs, 2), lax.rem(lax.div(fs, 2), 2), lax.div(fs, 4)
    heights = [lax.rem(y + step, 4) for step in (0, 3, 1, 2)]
    return [2 * h + side for h in heights] + [2 * h + 1 - side for h in heights], core


def in_vmem(arrays):
    return tuple(pltpu.with_memory_space_constraint(a, pltpu.VMEM) for a in arrays)


CHIPS = 4
COLUMNS = 256
DOWN_LIMIT = 6 << 20
SMALL_LIMIT = 4 << 20


def gate_value_kernel(chips, count, split, begun, ended, *refs):
    tokens, refs = refs[:count], refs[count:]
    weights = []
    for is_split in split:
        taken = 2 if is_split else 1
        weights.append(refs[:taken])
        refs = refs[taken:]
    before, refs = (refs[:2], refs[2:]) if begun else ((), refs)
    hidden, sums = (refs[0], refs[1:]) if ended else (None, refs)
    place, core = places()
    half = weights[0][0].shape[0] // 2
    width = weights[0][0].shape[1]

    def rows(i, which, at):
        if len(weights[i]) == 2:
            return weights[i][which][:, at]
        return weights[i][0][which * half : (which + 1) * half, at]

    for start in range(0, len(chips), CHIPS):
        sides = [(i, part) for i in range(start, start + CHIPS) for part in range(2)]
        blocks = []
        for i, part in sides:
            side = core if part == 0 else 1 - core
            at = pl.ds(pl.multiple_of((place[chips[i]] * 2 + side) * half, half), half)
            blocks.append(jnp.concatenate([t[:, at] for t in tokens], axis=0))
        block = jnp.concatenate(blocks, axis=1)
        held = sums if start > 0 else before
        final = ended and start + CHIPS == len(chips)

        def columns(k, carry, sides=sides, block=block, held=held, final=final):
            at = pl.ds(pl.multiple_of(k * COLUMNS, COLUMNS), COLUMNS)
            gate = jnp.concatenate([rows(2 * i + part, 0, at) for i, part in sides], axis=0)
            value = jnp.concatenate([rows(2 * i + part, 1, at) for i, part in sides], axis=0)
            gate = jnp.dot(block, gate, preferred_element_type=F32)
            value = jnp.dot(block, value, preferred_element_type=F32)
            if held:
                gate = gate + held[0][:, at]
                value = value + held[1][:, at]
            if final:
                hidden[:, at] = (gate / (1.0 + jnp.exp(-gate)) * value).astype(BF16)
            else:
                sums[0][:, at] = gate
                sums[1][:, at] = value
            return carry

        lax.fori_loop(0, width // COLUMNS, columns, 0)


def gate_value(tokens, weights, chips=tuple(range(8)), before=(), ended=True, limit=0):
    rows = len(tokens) * tokens[0].shape[0]
    weights = [weights[2 * j + part] for j in chips for part in range(2)]
    split = tuple(isinstance(w, tuple) for w in weights)
    flat = [a for w in weights for a in (w if isinstance(w, tuple) else (w,))]
    width = flat[0].shape[1]
    partial = [jax.ShapeDtypeStruct((rows, width), F32)] * 2
    out = [jax.ShapeDtypeStruct((rows, width), BF16)] if ended else partial
    held = ended and len(chips) > CHIPS
    args = (*in_vmem(tokens), *in_vmem(flat), *in_vmem(before))
    return pl.pallas_call(
        functools.partial(gate_value_kernel, chips, len(tokens), split, bool(before), ended),
        out_shape=out,
        in_specs=_vmem(len(args)),
        out_specs=_vmem(len(out)),
        scratch_shapes=[pltpu.VMEM((rows, width), F32)] * (2 if held else 0),
        compiler_params=pltpu.CompilerParams(vmem_limit_bytes=limit << 20),
        cost_estimate=pl.CostEstimate(
            flops=8 * rows * 128 * len(weights) * width, bytes_accessed=0, transcendentals=0
        ),
    )(*args)


def down_kernel(start, counts, split, hidden, *refs):
    weights = []
    for is_split in split:
        taken = 2 if is_split else 1
        weights.append(refs[:taken])
        refs = refs[taken:]
    added, outs = refs[: -len(counts)], refs[-len(counts) :]
    place, core = places()
    wide = weights[0][0].shape[1]
    block = hidden[start : start + sum(counts), :]
    for j in range(8):
        pair = [jnp.concatenate([w[...] for w in weights[2 * j + part]], axis=0) for part in range(2)]
        pair = jnp.concatenate(pair, axis=1)
        sums = jnp.dot(block, pair, preferred_element_type=F32)
        for part in range(2):
            side = core if part == 0 else 1 - core
            at = pl.ds(pl.multiple_of((place[j] * 2 + side) * wide, wide), wide)
            mine = sums[:, part * wide : (part + 1) * wide]
            row = 0
            for out, count in zip(outs, counts):
                rows = mine[row : row + count]
                if added:
                    low, high = rows[: count // 2], rows[count // 2 :]
                    if row == 0:
                        high = high + added[1][:, at].astype(F32)
                    else:
                        low = low + added[0][:, at].astype(F32)
                    rows = jnp.concatenate([low, high], axis=0)
                out[:, at] = rows.astype(out.dtype)
                row += count


def down(hidden, weights, start, outs, added=()):
    counts = tuple(rows for rows, _ in outs)
    wide = 16 * weights[0].shape[1]
    split = tuple(isinstance(w, tuple) for w in weights)
    flat = [a for w in weights for a in (w if isinstance(w, tuple) else (w,))]
    args = in_vmem((hidden, *flat, *added))
    return pl.pallas_call(
        functools.partial(down_kernel, start, counts, split),
        out_shape=[jax.ShapeDtypeStruct((rows, wide), t) for rows, t in outs],
        in_specs=_vmem(len(args)),
        out_specs=_vmem(len(outs)),
        compiler_params=pltpu.CompilerParams(vmem_limit_bytes=DOWN_LIMIT),
        cost_estimate=pl.CostEstimate(
            flops=2 * sum(counts) * hidden.shape[1] * wide, bytes_accessed=0, transcendentals=0
        ),
    )(*args)


def early_norm_kernel(tokens, norm, normed):
    normed[...] = rms(tokens[...], norm[...]).astype(BF16)


def add_kernel(over_low, under_high, low, high, over_out, under_out):
    over_out[...] = (over_low[...] + low[...].astype(F32)).astype(BF16)
    under_out[...] = (under_high[...] + high[...].astype(F32)).astype(BF16)


def _total(parts):
    total = parts[0][...]
    for part in parts[1:]:
        total = total + part.astype(F32)
    return total


def middle_kernel(own, p_low, p_high, m_low, m_high, tokens, mixer, post, mix, norm, mixed, normed):
    below = jnp.concatenate([p_low[...], p_high[...]], axis=0)
    above = jnp.concatenate([m_low[...], m_high[...]], axis=0)
    branch = rms(_total((own, below, above)), post[...])
    total = tokens[...].astype(F32) + 0.5 * branch + rms(mixer[...], mix[...])
    rounded = total.astype(BF16)
    mixed[...] = rounded
    normed[...] = rms(rounded, norm[...]).astype(BF16)


def last_kernel(p0, p1, p2, mixed, post, out):
    branch = rms(_total((p0, p1[...], p2[...])), post[...])
    out[...] = (mixed[...].astype(F32) + 0.5 * branch).astype(BF16)


def simple(kernel, shape, outs, *args):
    shapes = [jax.ShapeDtypeStruct(shape, BF16)] * outs
    return pl.pallas_call(
        kernel,
        out_shape=shapes,
        in_specs=_vmem(len(args)),
        out_specs=_vmem(outs),
        compiler_params=pltpu.CompilerParams(vmem_limit_bytes=SMALL_LIMIT),
    )(*args)


def join_kernel(gate, value, joined, sems):
    rows = gate.shape[0]
    first = pltpu.make_async_copy(gate, joined.at[pl.ds(0, rows), :], sems.at[0])
    second = pltpu.make_async_copy(value, joined.at[pl.ds(rows, rows), :], sems.at[1])
    first.start()
    second.start()
    first.wait()
    second.wait()


def join(gate, value):
    rows, width = gate.shape
    return pl.pallas_call(
        join_kernel,
        out_shape=jax.ShapeDtypeStruct((2 * rows, width), BF16),
        in_specs=[pl.BlockSpec(memory_space=pltpu.HBM)] * 2,
        out_specs=pl.BlockSpec(memory_space=pltpu.VMEM),
        scratch_shapes=[pltpu.SemaphoreType.DMA((2,))],
        compiler_params=pltpu.CompilerParams(vmem_limit_bytes=SMALL_LIMIT),
    )(*(pltpu.with_memory_space_constraint(a, pltpu.HBM) for a in (gate, value)))


def on_device(
    tokens,
    mixer_output,
    early_norm,
    early_gate,
    early_value,
    early_down,
    early_post,
    mixer_gain,
    later_norm,
    later_gate,
    later_value,
    later_down,
    later_post,
):
    early_wide = all_pieces(join(early_gate, early_value), "++--")
    early_low = all_pieces(early_down, "-++-", turned=True)
    later_wide = all_pieces(join(later_gate, later_value), "++-", halved=True)
    later_low = all_pieces(later_down, "-+++", turned=True)
    shape = tokens.shape

    def gathered(normed):
        across = z_shift(2)(normed)
        under = z_shift(1)(normed)
        over = z_shift(-1)(normed)
        return across, normed, under, over

    half, whole = shape[0] // 2, shape[0]
    far = ((half, BF16), (half, BF16), (whole, F32))
    near = ((whole, BF16), (whole, BF16))

    def passed_on(low, high):
        return z_shift(1)(low), z_shift(-1)(high)

    def returned(under, over):
        return z_shift(1)(over), z_shift(-1)(under)

    (early_in,) = simple(early_norm_kernel, shape, 1, tokens, early_norm[None])
    rows = gathered(early_in)
    sums = gate_value(rows, early_wide, (0, 3, 4, 7), ended=False, limit=18)
    (hidden,) = gate_value(rows, early_wide, (1, 2, 5, 6), sums, limit=18)
    low, high, own = down(hidden, early_low, 0, far)
    added = passed_on(low, high)
    quarter = ((half, BF16), (half, F32), (half, F32), (half, BF16))
    under_low, under_high, over_low, over_high = down(hidden, early_low, 2 * whole, quarter)
    p_high, m_low = z_shift(1)(over_high), z_shift(-1)(under_low)
    over_low, under_high = simple(add_kernel, (half, shape[1]), 2, over_low, under_high, *added)
    p_low, m_high = z_shift(1)(over_low), z_shift(-1)(under_high)
    parts = (own, p_low, p_high, m_low, m_high)
    gains = (early_post[None], mixer_gain[None], later_norm[None])
    mixed, later_in = simple(middle_kernel, shape, 2, *parts, tokens, mixer_output, *gains)
    rows = gathered(later_in)
    across, own, under, over = rows
    (hidden,) = gate_value((across,), later_wide, limit=8)
    low, high = down(hidden, later_low, 0, far[:2])
    added = passed_on(low, high)
    (hidden,) = gate_value((under, over, own), later_wide, limit=8)
    near_sums = down(hidden, later_low, 0, near, added)
    (own,) = down(hidden, later_low, 2 * whole, far[2:])
    parts = (own, *returned(*near_sums))
    (out,) = simple(last_kernel, shape, 1, *parts, mixed, later_post[None])
    return out


def solution(mesh):
    placed = (
        P(("rep", "fs", "tp"), None),
        P(("rep", "fs", "tp"), None),
        P(),
        P("fs", "tp"),
        P("fs", "tp"),
        P("tp", "fs"),
        P(),
        P(),
        P(),
        P("fs", "tp"),
        P("fs", "tp"),
        P("tp", "fs"),
        P(),
    )
    return jax.shard_map(
        on_device,
        mesh=mesh,
        in_specs=placed,
        out_specs=P(("rep", "fs", "tp"), None),
        check_vma=False,
    )
```

```python
import functools

import jax
import jax.numpy as jnp
from jax import lax
from jax.experimental import pallas as pl
from jax.experimental.pallas import tpu as pltpu
from jax.sharding import PartitionSpec as P


epsilon = 1e-06
PLANE = ("rep", "fs")
F32 = jnp.float32
BF16 = jnp.bfloat16


def _place(x, y, core):
    return (x // 2) * 16 + y * 4 + (x % 2) * 2 + core


def _plane_shift(dx, dy, flip):
    pairs = []
    for x in range(4):
        for y in range(4):
            for core in range(2):
                there = _place((x + dx) % 4, (y + dy) % 4, core ^ flip)
                pairs.append((_place(x, y, core), there))
    return lambda a: lax.ppermute(a, PLANE, pairs)


y_up = _plane_shift(0, 1, 0)
y_down = _plane_shift(0, -1, 0)
y_across = _plane_shift(0, 2, 0)
x_up = _plane_shift(1, 0, 0)
x_down = _plane_shift(-1, 0, 0)
to_partner = _plane_shift(0, 0, 1)


def z_shift(step):
    return lambda a: lax.ppermute(a, "tp", [(i, (i + step) % 4) for i in range(4)])


def all_pieces(own, ways, halved=False, turned=False):
    below = y_up(own)
    above = y_down(own)
    across = y_across(own)
    pieces = [own, below, above, across]
    for i, way in enumerate(ways):
        send, piece = x_up if way == "+" else x_down, pieces[i]
        if turned and i in (1, 2):
            send, piece = (y_up, y_down)[i - 1], pieces[4]
        pieces.append(send(piece))
    out = []
    for piece in pieces:
        out += [piece, to_partner(piece)]
    if halved:
        gate, value = halve(across)
        last = (x_up(gate), x_down(value))
        out += [last, tuple(to_partner(a) for a in last)]
    return out


def halve_kernel(whole, low, high):
    rows = low.shape[0]
    low[...] = whole[:rows, :]
    high[...] = whole[rows:, :]


def halve(whole):
    half = (whole.shape[0] // 2, whole.shape[1])
    return simple(halve_kernel, half, 2, whole)


def rms(values, gain):
    values = values.astype(F32)
    scale = lax.rsqrt(jnp.mean(values * values, axis=-1, keepdims=True) + epsilon)
    return values * scale * gain


def _vmem(n):
    return [pl.BlockSpec(memory_space=pltpu.VMEM)] * n


def places():
    fs = lax.axis_index("fs")
    core, side, y = lax.rem(fs, 2), lax.rem(lax.div(fs, 2), 2), lax.div(fs, 4)
    heights = [lax.rem(y + step, 4) for step in (0, 3, 1, 2)]
    return [2 * h + side for h in heights] + [2 * h + 1 - side for h in heights], core


def in_vmem(arrays):
    return tuple(pltpu.with_memory_space_constraint(a, pltpu.VMEM) for a in arrays)


COLUMNS = 256
DOWN_LIMIT = 6 << 20
SMALL_LIMIT = 4 << 20


def gate_value_kernel(chips, count, split, begun, ended, *refs):
    tokens, refs = refs[:count], refs[count:]
    weights = []
    for is_split in split:
        taken = 2 if is_split else 1
        weights.append(refs[:taken])
        refs = refs[taken:]
    before, refs = (refs[:2], refs[2:]) if begun else ((), refs)
    hidden, sums = (refs[0], refs[1:]) if ended else (None, refs)
    place, core = places()
    half = weights[0][0].shape[0] // 2
    width = weights[0][0].shape[1]

    def rows(i, which, at):
        if len(weights[i]) == 2:
            return weights[i][which][:, at]
        return weights[i][0][which * half : (which + 1) * half, at]

    step = len(chips)
    for start in range(0, len(chips), step):
        sides = [(i, part) for i in range(start, start + step) for part in range(2)]
        blocks = []
        for i, part in sides:
            side = core if part == 0 else 1 - core
            at = pl.ds(pl.multiple_of((place[chips[i]] * 2 + side) * half, half), half)
            blocks.append(jnp.concatenate([t[:, at] for t in tokens], axis=0))
        block = jnp.concatenate(blocks, axis=1)
        held = sums if start > 0 else before
        final = ended and start + step == len(chips)

        def columns(k, carry, sides=sides, block=block, held=held, final=final):
            at = pl.ds(pl.multiple_of(k * COLUMNS, COLUMNS), COLUMNS)
            gate = jnp.concatenate([rows(2 * i + part, 0, at) for i, part in sides], axis=0)
            value = jnp.concatenate([rows(2 * i + part, 1, at) for i, part in sides], axis=0)
            gate = jnp.dot(block, gate, preferred_element_type=F32)
            value = jnp.dot(block, value, preferred_element_type=F32)
            if held:
                gate = gate + held[0][:, at]
                value = value + held[1][:, at]
            if final:
                hidden[:, at] = (gate / (1.0 + jnp.exp(-gate)) * value).astype(BF16)
            else:
                sums[0][:, at] = gate
                sums[1][:, at] = value
            return carry

        lax.fori_loop(0, width // COLUMNS, columns, 0)


def gate_value(tokens, weights, chips=tuple(range(8)), before=(), ended=True, limit=0):
    rows = len(tokens) * tokens[0].shape[0]
    weights = [weights[2 * j + part] for j in chips for part in range(2)]
    split = tuple(isinstance(w, tuple) for w in weights)
    flat = [a for w in weights for a in (w if isinstance(w, tuple) else (w,))]
    width = flat[0].shape[1]
    partial = [jax.ShapeDtypeStruct((rows, width), F32)] * 2
    out = [jax.ShapeDtypeStruct((rows, width), BF16)] if ended else partial
    held = False
    args = (*in_vmem(tokens), *in_vmem(flat), *in_vmem(before))
    return pl.pallas_call(
        functools.partial(gate_value_kernel, chips, len(tokens), split, bool(before), ended),
        out_shape=out,
        in_specs=_vmem(len(args)),
        out_specs=_vmem(len(out)),
        scratch_shapes=[pltpu.VMEM((rows, width), F32)] * (2 if held else 0),
        compiler_params=pltpu.CompilerParams(vmem_limit_bytes=limit << 20),
        cost_estimate=pl.CostEstimate(
            flops=8 * rows * 128 * len(weights) * width, bytes_accessed=0, transcendentals=0
        ),
    )(*args)


def down_kernel(start, counts, split, hidden, *refs):
    weights = []
    for is_split in split:
        taken = 2 if is_split else 1
        weights.append(refs[:taken])
        refs = refs[taken:]
    added, outs = refs[: -len(counts)], refs[-len(counts) :]
    place, core = places()
    wide = weights[0][0].shape[1]
    block = hidden[start : start + sum(counts), :]
    for j in range(8):
        pair = [jnp.concatenate([w[...] for w in weights[2 * j + part]], axis=0) for part in range(2)]
        pair = jnp.concatenate(pair, axis=1)
        sums = jnp.dot(block, pair, preferred_element_type=F32)
        for part in range(2):
            side = core if part == 0 else 1 - core
            at = pl.ds(pl.multiple_of((place[j] * 2 + side) * wide, wide), wide)
            mine = sums[:, part * wide : (part + 1) * wide]
            row = 0
            for out, count in zip(outs, counts):
                rows = mine[row : row + count]
                if added:
                    low, high = rows[: count // 2], rows[count // 2 :]
                    if row == 0:
                        high = high + added[1][:, at].astype(F32)
                    else:
                        low = low + added[0][:, at].astype(F32)
                    rows = jnp.concatenate([low, high], axis=0)
                out[:, at] = rows.astype(out.dtype)
                row += count


def down(hidden, weights, start, outs, added=()):
    counts = tuple(rows for rows, _ in outs)
    wide = 16 * weights[0].shape[1]
    split = tuple(isinstance(w, tuple) for w in weights)
    flat = [a for w in weights for a in (w if isinstance(w, tuple) else (w,))]
    args = in_vmem((hidden, *flat, *added))
    return pl.pallas_call(
        functools.partial(down_kernel, start, counts, split),
        out_shape=[jax.ShapeDtypeStruct((rows, wide), t) for rows, t in outs],
        in_specs=_vmem(len(args)),
        out_specs=_vmem(len(outs)),
        compiler_params=pltpu.CompilerParams(vmem_limit_bytes=DOWN_LIMIT),
        cost_estimate=pl.CostEstimate(
            flops=2 * sum(counts) * hidden.shape[1] * wide, bytes_accessed=0, transcendentals=0
        ),
    )(*args)


def early_norm_kernel(tokens, norm, normed):
    normed[...] = rms(tokens[...], norm[...]).astype(BF16)


def add_kernel(over_low, under_high, low, high, over_out, under_out):
    over_out[...] = (over_low[...] + low[...].astype(F32)).astype(BF16)
    under_out[...] = (under_high[...] + high[...].astype(F32)).astype(BF16)


def _total(parts):
    total = parts[0][...]
    for part in parts[1:]:
        total = total + part.astype(F32)
    return total


def middle_kernel(own, p_low, p_high, m_low, m_high, tokens, mixer, post, mix, norm, mixed, normed):
    below = jnp.concatenate([p_low[...], p_high[...]], axis=0)
    above = jnp.concatenate([m_low[...], m_high[...]], axis=0)
    branch = rms(_total((own, below, above)), post[...])
    total = tokens[...].astype(F32) + 0.5 * branch + rms(mixer[...], mix[...])
    rounded = total.astype(BF16)
    mixed[...] = rounded
    normed[...] = rms(rounded, norm[...]).astype(BF16)


def last_kernel(p0, p1, p2, mixed, post, out):
    branch = rms(_total((p0, p1[...], p2[...])), post[...])
    out[...] = (mixed[...].astype(F32) + 0.5 * branch).astype(BF16)


def simple(kernel, shape, outs, *args):
    shapes = [jax.ShapeDtypeStruct(shape, BF16)] * outs
    return pl.pallas_call(
        kernel,
        out_shape=shapes,
        in_specs=_vmem(len(args)),
        out_specs=_vmem(outs),
        compiler_params=pltpu.CompilerParams(vmem_limit_bytes=SMALL_LIMIT),
    )(*args)


def join_kernel(gate, value, joined, sems):
    rows = gate.shape[0]
    first = pltpu.make_async_copy(gate, joined.at[pl.ds(0, rows), :], sems.at[0])
    second = pltpu.make_async_copy(value, joined.at[pl.ds(rows, rows), :], sems.at[1])
    first.start()
    second.start()
    first.wait()
    second.wait()


def join(gate, value):
    rows, width = gate.shape
    return pl.pallas_call(
        join_kernel,
        out_shape=jax.ShapeDtypeStruct((2 * rows, width), BF16),
        in_specs=[pl.BlockSpec(memory_space=pltpu.HBM)] * 2,
        out_specs=pl.BlockSpec(memory_space=pltpu.VMEM),
        scratch_shapes=[pltpu.SemaphoreType.DMA((2,))],
        compiler_params=pltpu.CompilerParams(vmem_limit_bytes=SMALL_LIMIT),
    )(*(pltpu.with_memory_space_constraint(a, pltpu.HBM) for a in (gate, value)))


def on_device(
    tokens,
    mixer_output,
    early_norm,
    early_gate,
    early_value,
    early_down,
    early_post,
    mixer_gain,
    later_norm,
    later_gate,
    later_value,
    later_down,
    later_post,
):
    early_wide = all_pieces(join(early_gate, early_value), "++--")
    early_low = all_pieces(early_down, "-++-", turned=True)
    later_wide = all_pieces(join(later_gate, later_value), "++-", halved=True)
    later_low = all_pieces(later_down, "-+++", turned=True)
    shape = tokens.shape

    def gathered(normed):
        across = z_shift(2)(normed)
        under = z_shift(1)(normed)
        over = z_shift(-1)(normed)
        return across, normed, under, over

    half, whole = shape[0] // 2, shape[0]
    far = ((half, BF16), (half, BF16), (whole, F32))
    near = ((whole, BF16), (whole, BF16))

    def passed_on(low, high):
        return z_shift(1)(low), z_shift(-1)(high)

    def returned(under, over):
        return z_shift(1)(over), z_shift(-1)(under)

    (early_in,) = simple(early_norm_kernel, shape, 1, tokens, early_norm[None])
    rows = gathered(early_in)
    sums = gate_value(rows, early_wide, (0, 3, 4, 7), ended=False, limit=18)
    (hidden,) = gate_value(rows, early_wide, (1, 2, 5, 6), sums, limit=18)
    low, high, own = down(hidden, early_low, 0, far)
    added = passed_on(low, high)
    quarter = ((half, BF16), (half, F32), (half, F32), (half, BF16))
    under_low, under_high, over_low, over_high = down(hidden, early_low, 2 * whole, quarter)
    p_high, m_low = z_shift(1)(over_high), z_shift(-1)(under_low)
    over_low, under_high = simple(add_kernel, (half, shape[1]), 2, over_low, under_high, *added)
    p_low, m_high = z_shift(1)(over_low), z_shift(-1)(under_high)
    parts = (own, p_low, p_high, m_low, m_high)
    gains = (early_post[None], mixer_gain[None], later_norm[None])
    mixed, later_in = simple(middle_kernel, shape, 2, *parts, tokens, mixer_output, *gains)
    rows = gathered(later_in)
    across, own, under, over = rows
    (hidden,) = gate_value((across,), later_wide, limit=8)
    low, high = down(hidden, later_low, 0, far[:2])
    added = passed_on(low, high)
    (hidden,) = gate_value((under, over, own), later_wide, limit=8)
    near_sums = down(hidden, later_low, 0, near, added)
    (own,) = down(hidden, later_low, 2 * whole, far[2:])
    parts = (own, *returned(*near_sums))
    (out,) = simple(last_kernel, shape, 1, *parts, mixed, later_post[None])
    return out


def solution(mesh):
    placed = (
        P(("rep", "fs", "tp"), None),
        P(("rep", "fs", "tp"), None),
        P(),
        P("fs", "tp"),
        P("fs", "tp"),
        P("tp", "fs"),
        P(),
        P(),
        P(),
        P("fs", "tp"),
        P("fs", "tp"),
        P("tp", "fs"),
        P(),
    )
    return jax.shard_map(
        on_device,
        mesh=mesh,
        in_specs=placed,
        out_specs=P(("rep", "fs", "tp"), None),
        check_vma=False,
    )
```
